32 devices in a mesh: sp: 16 (over z, y, x), tp: 2 (over core).
Axes of the slice: x: 2, y: 2, z: 4, core: 2. Of those that a mesh axis runs over, the one named last changes fastest.
Arguments:
- stream: bfloat16 [6144, 2048], P('sp', 'tp'), may hold values from -6 to 6
- norm_gain: float32 [2, 2048], replicated, may hold values from 0.1 to 1.9
- a_weight: bfloat16 [2, 2048, 2048], P(None, 'sp', 'tp'), may hold values from -0.125 to 0.125
- gate_weight: bfloat16 [2, 2048, 2048], P(None, 'sp', 'tp'), may hold values from -0.125 to 0.125
- conv_weight: float32 [2, 31, 2048], P(None, None, 'tp'), may hold values from -4 to 4, as said below
- conv_bias: float32 [2, 2048], P(None, 'tp'), may hold values from -3 to 3
- ln_gain: float32 [2, 2048], P(None, 'tp'), may hold values from 0.1 to 1.9
- ln_shift: float32 [2, 2048], P(None, 'tp'), may hold values from -3 to 3
- out_weight: bfloat16 [2, 2048, 2048], P(None, 'sp', 'tp'), may hold values from -0.125 to 0.125
Outputs:
- result: bfloat16 [6144, 2048], P('sp', 'tp')
The draws below stay inside these ranges and needn't reach their ends.
Inputs may be any that keep to these rules, and one draw needn't show every extreme that they name: `conv_weight`: each column is drawn with its own scale, and blocks of 16 channels differ in scale by up to a factor of nine.
All inputs are finite; a program needn't handle non-finite values.
Results may differ from the reference program's by a relative error of at most 0.01.
Values may be sent and summed in bfloat16 or wider, within the bound.
A program may use at most 64 MiB of HBM per device.

```python
import jax
import jax.numpy as jnp
from jax import lax

D = 2048
WIDTH = 31
LAYERS = 2
TOKENS = 6144


def draw_conv_weight(key, part):
    first = jax.random.fold_in(key, 11)
    second = jax.random.fold_in(key, 12)
    values = jnp.clip(jax.random.normal(first, (LAYERS, WIDTH, D), jnp.float32), -6.0, 6.0)
    block_scale = jnp.exp(jax.random.uniform(second, (LAYERS, 1, D // 16), jnp.float32, -1.09, 1.09))
    spread_scale = jnp.repeat(block_scale, 16, axis=2)
    return values * spread_scale * WIDTH ** (-0.5)


def shard_levels(key, shape, cuts, smallest, high):
    level = 1.0
    for dim, blocks in cuts:
        steps = jax.random.uniform(jax.random.fold_in(jax.random.fold_in(key, 6), dim), (blocks,), jnp.float32, smallest / len(cuts), high / len(cuts))
        level = level * jnp.repeat(jnp.exp(steps), shape[dim] // blocks).reshape((-1,) + (1,) * (len(shape) - 1 - dim))
    return level


def normal_values(stream_key, dims, spread, most, shards=(), kind=jnp.bfloat16):
    drawn = jax.random.normal(stream_key, dims, jnp.float32) * spread
    if len(shards) > 0:
        drawn = shard_levels(stream_key, dims, shards, -0.22, 0.18) * drawn
    return jnp.clip(drawn, min=-most, max=most).astype(kind)


def setup_inputs(seed: int = 0) -> dict:
    arg_keys = jax.random.split(jax.random.key(seed), 10)
    return {
        "stream": normal_values(arg_keys[0], (TOKENS, D), 1.0, 6.0, ((0, 16), (1, 2))),
        "norm_gain": jnp.clip(1.0 + 0.18 * jax.random.normal(arg_keys[1], (LAYERS, D), jnp.float32), 0.1, 1.9),
        "a_weight": normal_values(arg_keys[2], (LAYERS, D, D), D ** -0.5, 0.125, ((1, 16), (2, 2))),
        "gate_weight": normal_values(arg_keys[3], (LAYERS, D, D), D ** -0.5, 0.125, ((1, 16), (2, 2))),
        "conv_weight": draw_conv_weight(jax.random.fold_in(arg_keys[9], 71), 0),
        "conv_bias": normal_values(arg_keys[5], (LAYERS, D), 0.5, 3.0, ((1, 2),), jnp.float32),
        "ln_gain": jnp.clip(1.0 + 0.18 * jax.random.normal(arg_keys[6], (LAYERS, D), jnp.float32), 0.1, 1.9),
        "ln_shift": normal_values(arg_keys[7], (LAYERS, D), 0.5, 3.0, ((1, 2),), jnp.float32),
        "out_weight": normal_values(arg_keys[8], (LAYERS, D, D), D ** -0.5, 0.125, ((1, 16), (2, 2))),
    }


EPSILON = 1e-06

def normalize_rows(stream_f, gain):
    factor = lax.rsqrt(lax.optimization_barrier(jnp.mean(stream_f * stream_f, axis=1, keepdims=True)) + EPSILON)
    return (stream_f * factor * gain[None, :]).astype(jnp.bfloat16)

def convolve(padded, kernel, conv_shift, out_rows):
    summed = jnp.zeros((out_rows, padded.shape[1]), jnp.float32) + conv_shift[None, :]
    for offset in range(kernel.shape[0]):
        window = lax.slice_in_dim(padded, offset, offset + out_rows, axis=0).astype(jnp.float32)
        summed = summed + window * kernel[offset][None, :]
    return summed

def finish_norm(conv_out, row_sum, row_squares, gain, shift):
    average = row_sum / D
    variance = row_squares / D - average * average
    normed = (conv_out - average) * lax.rsqrt(variance + EPSILON) * gain[None, :] + shift[None, :]
    return jax.nn.silu(normed).astype(jnp.bfloat16)

def reference(stream, norm_gain, a_weight, gate_weight, conv_weight, conv_bias, ln_gain, ln_shift, out_weight):
    reach = (WIDTH - 1) // 2
    current = stream
    for layer_index in range(LAYERS):
        stream_f = current.astype(jnp.float32)
        normed = normalize_rows(stream_f, norm_gain[layer_index])
        linear = jnp.dot(normed, a_weight[layer_index], preferred_element_type=jnp.float32)
        gating = jnp.dot(normed, gate_weight[layer_index], preferred_element_type=jnp.float32)
        gated = (linear * jax.nn.sigmoid(gating)).astype(jnp.bfloat16)
        padded = jnp.pad(gated, ((reach, reach), (0, 0)))
        conv_out = convolve(padded, conv_weight[layer_index], conv_bias[layer_index], TOKENS)
        row_sum = lax.optimization_barrier(jnp.sum(conv_out, axis=1, keepdims=True))
        row_squares = lax.optimization_barrier(jnp.sum(conv_out * conv_out, axis=1, keepdims=True))
        mixed_in = finish_norm(conv_out, row_sum, row_squares, ln_gain[layer_index], ln_shift[layer_index])
        branch = jnp.dot(mixed_in, out_weight[layer_index], preferred_element_type=jnp.float32)
        current = (stream_f + branch).astype(jnp.bfloat16)
    return current
```

```python
import functools

import jax
import jax.numpy as jnp
from jax import lax
from jax.experimental import pallas as pl
from jax.experimental.pallas import tpu as pltpu
from jax.sharding import PartitionSpec as P

D = 2048


EPSILON = 1e-06
MESH = pl.DeviceIdType.MESH
LOOKAHEAD = 3
ROUND = 16
HALVES = 2
ORDERS = ((0, 1, 2), (0, 2, 1))
LANES = 128
CUTS = 2
VMEM_BYTES = 60 * 2**20


def grid_of(mesh):
    count = mesh.shape["sp"]
    row = mesh.devices[:, 0]
    coords = [getattr(device, "coords", None) for device in row]
    if any(c is None for c in coords):
        return (count // 4, 2, 2) if count % 4 == 0 else (count, 1, 1)
    sizes = tuple(len({c[axis] for c in coords}) for axis in (2, 1, 0))
    if sizes[0] * sizes[1] * sizes[2] != count:
        return (count, 1, 1)
    return sizes


def gather_kernel(sizes, pieces, count, *refs):
    ins, outs = refs[:count], refs[count:-3]
    local_sem, send_sem, recv_sem = refs[-3:]
    me = lax.axis_index("sp")
    strides = (sizes[1] * sizes[2], sizes[2], 1)
    where = [lax.rem(me // strides[k], sizes[k]) for k in range(3)]
    wide = ins[0].shape[2] // HALVES

    def peer(axis, step):
        other = lax.rem(where[axis] + step, sizes[axis])
        return me + (other - where[axis]) * strides[axis]

    peers = [(axis, step) for axis in range(3) for step in range(1, sizes[axis])]
    barrier = pltpu.get_barrier_semaphore()
    for axis, step in peers:
        pl.semaphore_signal(barrier, inc=1, device_id={"sp": peer(axis, step)}, device_id_type=MESH)
    pl.semaphore_wait(barrier, len(peers))

    def source(piece):
        matrix, layer, half = pieces[piece][:3]
        return ins[matrix].at[layer, :, pl.ds(half * wide, wide)]

    def block(piece, done):
        half, phases, out, slot = pieces[piece][2:]
        order = ORDERS[half]
        if phases == 3:
            index = [slice(None) if axis in done else where[axis] for axis in range(3)]
            return outs[out].at[(*index, slice(None), pl.ds(half * wide, wide))]
        index = [slice(None) if axis in done else where[axis] for axis in order[:2]]
        return outs[out].at[(slot, *index, slice(None), slice(None))]

    def local(piece):
        return pltpu.make_async_copy(source(piece), block(piece, ()), local_sem.at[piece])

    def copies(piece, phase):
        order = ORDERS[pieces[piece][2]]
        if phase >= pieces[piece][3]:
            return []
        axis = order[phase]
        target = block(piece, order[:phase])
        found = []
        for step in range(1, sizes[axis]):
            slot = peers.index((axis, step))
            found.append(
                pltpu.make_async_remote_copy(
                    src_ref=source(piece) if phase == 0 else target,
                    dst_ref=target,
                    send_sem=send_sem.at[piece, slot],
                    recv_sem=recv_sem.at[piece, slot],
                    device_id={"sp": peer(axis, step)},
                    device_id_type=MESH,
                )
            )
        return found

    def start(piece, phase):
        if phase == 0:
            local(piece).start()
        for copy in copies(piece, phase):
            copy.start()

    def landed(piece, phase):
        if phase == 0:
            local(piece).wait()
        for copy in copies(piece, phase):
            copy.wait_recv()

    total = len(pieces)
    for piece in range(min(LOOKAHEAD, total)):
        start(piece, 0)
    for step in range(total + 1):
        if step + LOOKAHEAD < total:
            start(step + LOOKAHEAD, 0)
        if step < total:
            landed(step, 0)
            start(step, 1)
        if step >= 1:
            landed(step - 1, 1)
            start(step - 1, 2)
    for piece in range(total):
        landed(piece, 2)
        for phase in range(3):
            for copy in copies(piece, phase):
                copy.wait_send()


def gather_weights(sizes, weights, deferred):
    layers, depth, columns = weights[0].shape
    whole = layers - 1 if deferred else layers
    shapes, pieces = [], []
    for layer in range(whole):
        for matrix in range(3):
            for half in range(HALVES):
                pieces.append((matrix, layer, half, 3, len(shapes), 0))
            shapes.append((*sizes, depth, columns))
    if deferred:
        base = len(shapes)
        for group, members in enumerate(((0, 1), (2,))):
            for half in range(HALVES):
                ahead = tuple(sizes[axis] for axis in ORDERS[half][:2])
                shapes.append((len(members), *ahead, depth, columns // HALVES))
            for slot, matrix in enumerate(members):
                for half in range(HALVES):
                    out = base + group * HALVES + half
                    pieces.append((matrix, whole, half, 2, out, slot))
    slots = sum(size - 1 for size in sizes)
    gathered = pl.pallas_call(
        functools.partial(gather_kernel, sizes, pieces, len(weights)),
        out_shape=[jax.ShapeDtypeStruct(shape, jnp.bfloat16) for shape in shapes],
        in_specs=[pl.BlockSpec(memory_space=pltpu.VMEM)] * len(weights),
        out_specs=[pl.BlockSpec(memory_space=pl.ANY)] * len(shapes),
        scratch_shapes=[
            pltpu.SemaphoreType.DMA((len(pieces),)),
            pltpu.SemaphoreType.DMA((len(pieces), slots)),
            pltpu.SemaphoreType.DMA((len(pieces), slots)),
        ],
        compiler_params=pltpu.CompilerParams(collective_id=0, has_side_effects=True),
    )(*weights)
    rows = sizes[0] * sizes[1] * sizes[2] * depth
    full = [gathered[k].reshape(rows, columns) for k in range(3 * whole)]
    return full, gathered[3 * whole :]


def last_hop(stage, sizes, half):
    axis = ORDERS[half][2]
    stride = (sizes[1] * sizes[2], sizes[2], 1)[axis]
    count = sizes[0] * sizes[1] * sizes[2]
    pairs = [(i, i + stride if (i // stride) % 2 == 0 else i - stride) for i in range(count)]
    return lax.ppermute(stage, "sp", pairs)


def split_channels(block, sizes, half):
    axis = ORDERS[half][2]
    count = sizes[0] * sizes[1] * sizes[2]
    depth = block.shape[1] // count
    stride = (sizes[1] * sizes[2], sizes[2], 1)[axis]
    sides = [
        jnp.concatenate(
            [block[:, i * depth : (i + 1) * depth] for i in range(count) if (i // stride) % 2 == side],
            axis=1,
        )
        for side in range(2)
    ]
    first = lax.rem(lax.axis_index("sp") // stride, 2) == 0
    return jnp.where(first, sides[0], sides[1]), jnp.where(first, sides[1], sides[0])


def split_dot(parts, own, other):
    return jnp.dot(
        parts[0], own.reshape(-1, own.shape[-1]), preferred_element_type=jnp.float32
    ) + jnp.dot(parts[1], other.reshape(-1, other.shape[-1]), preferred_element_type=jnp.float32)


def with_halo(block, width):
    count = lax.axis_size("sp")
    forward = [(i, i + 1) for i in range(count - 1)]
    backward = [(target, source) for source, target in forward]
    low = lax.ppermute(block[block.shape[0] - width :], "sp", forward)
    high = lax.ppermute(block[:width], "sp", backward)
    return jnp.concatenate([low, block, high], axis=0)


def all_channels(block):
    if lax.axis_size("tp") != 2:
        return lax.all_gather(block, "tp", axis=1, tiled=True)
    other = lax.ppermute(block, "tp", [(0, 1), (1, 0)])
    first = lax.axis_index("tp") == 0
    return jnp.concatenate(
        [jnp.where(first, block, other), jnp.where(first, other, block)], axis=1
    )


def normalize_rows(stream_f, gain):
    factor = lax.rsqrt(jnp.mean(stream_f * stream_f, axis=1, keepdims=True) + EPSILON)
    return (stream_f * factor * gain[None, :]).astype(jnp.bfloat16)


def convolve(padded, kernel, conv_shift, out_rows):
    summed = jnp.zeros((out_rows, padded.shape[1]), jnp.float32) + conv_shift[None, :]
    for offset in range(kernel.shape[0]):
        window = lax.slice_in_dim(padded, offset, offset + out_rows, axis=0).astype(jnp.float32)
        summed = summed + window * kernel[offset][None, :]
    return summed


def finish_norm(conv_out, row_sum, row_squares, gain, shift):
    average = row_sum / D
    variance = row_squares / D - average * average
    normed = (conv_out - average) * lax.rsqrt(variance + EPSILON) * gain[None, :] + shift[None, :]
    return jax.nn.silu(normed).astype(jnp.bfloat16)


def local(
    sizes,
    stream,
    norm_gain,
    a_weight,
    gate_weight,
    conv_weight,
    conv_bias,
    ln_gain,
    ln_shift,
    out_weight,
):
    reach = (conv_weight.shape[1] - 1) // 2
    margin = (reach + ROUND - 1) // ROUND * ROUND
    layer_total = a_weight.shape[0]
    rows = stream.shape[0]
    deferred = sizes[1] == 2 and sizes[2] == 2 and layer_total > 1
    full, stages = gather_weights(sizes, (a_weight, gate_weight, out_weight), deferred)
    hops = []
    token = lax.axis_index("sp") * rows
    everything = rows * lax.axis_size("sp")
    spread = with_halo(all_channels(stream), margin * layer_total)
    wide = stream.shape[1]
    current = lax.dynamic_slice_in_dim(spread, lax.axis_index("tp") * wide, wide, axis=1)
    for layer_index in range(layer_total):
        beyond = margin * (layer_total - layer_index)
        if layer_index > 0:
            index = token - beyond + lax.broadcasted_iota(jnp.int32, (current.shape[0], 1), 0)
            inside = (index >= 0) & (index < everything)
            current = jnp.where(inside, current, jnp.zeros_like(current))
            spread = all_channels(current)
        stream_f = current.astype(jnp.float32)
        normed = normalize_rows(spread.astype(jnp.float32), norm_gain[layer_index])
        late = deferred and layer_index == layer_total - 1
        if late:
            gated = []
            for half in range(HALVES):
                parts = split_channels(normed, sizes, half)
                own, other = stages[half], hops[half]
                linear = split_dot(parts, own[0], other[0])
                gating = split_dot(parts, own[1], other[1])
                gated.append((linear * jax.nn.sigmoid(gating)).astype(jnp.bfloat16))
            gated = jnp.concatenate(gated, axis=1)
        else:
            matrices = full[3 * layer_index : 3 * layer_index + 3]
            linear = jnp.dot(normed, matrices[0], preferred_element_type=jnp.float32)
            gating = jnp.dot(normed, matrices[1], preferred_element_type=jnp.float32)
            gated = (linear * jax.nn.sigmoid(gating)).astype(jnp.bfloat16)
        if deferred and layer_index == layer_total - 2:
            hops = [last_hop(stages[half], sizes, half) for half in range(HALVES)]
            hops += [last_hop(stages[HALVES + half], sizes, half) for half in range(HALVES)]
        out_rows = rows + 2 * (beyond - margin)
        conv_out = convolve(
            gated[margin - reach :], conv_weight[layer_index], conv_bias[layer_index], out_rows
        )
        row_sum, row_squares = lax.psum(
            (
                jnp.sum(conv_out, axis=1, keepdims=True),
                jnp.sum(conv_out * conv_out, axis=1, keepdims=True),
            ),
            "tp",
        )
        mixed_in = finish_norm(
            conv_out, row_sum, row_squares, ln_gain[layer_index], ln_shift[layer_index]
        )
        mixed_rows = all_channels(mixed_in)
        if late:
            branch = jnp.concatenate(
                [
                    split_dot(
                        split_channels(mixed_rows, sizes, half),
                        stages[HALVES + half][0],
                        hops[HALVES + half][0],
                    )
                    for half in range(HALVES)
                ],
                axis=1,
            )
        else:
            branch = jnp.dot(mixed_rows, matrices[2], preferred_element_type=jnp.float32)
        kept = lax.slice_in_dim(stream_f, margin, margin + out_rows, axis=0)
        current = (kept + branch).astype(jnp.bfloat16)
    return current


RELATIONS = 3


def fused_kernel(
    sizes,
    layers,
    taps,
    stream,
    norm_gain,
    a_weight,
    gate_weight,
    out_weight,
    conv_weight,
    conv_bias,
    ln_gain,
    ln_shift,
    out,
    weights,
    spread,
    normed,
    gated,
    conv_out,
    final,
    taps_own,
    cols_own,
    sums_own,
    sums_in,
    *rest,
):
    inner = rest[: layers - 1]
    mixed = rest[layers - 1 : 2 * layers - 1]
    sems = rest[2 * layers - 1 :]
    (w_local, w_send, w_recv, x_local, x_send, x_recv, s_send, s_recv, m_send, m_recv, c_send, c_recv, f_send, f_recv) = sems
    depth_z, width_y, width_x = sizes
    plane = width_y * width_x
    count = depth_z * plane
    rows, wide = stream.shape
    total = 2 * wide
    half = wide // 2
    depth = a_weight.shape[1]
    reach = (taps - 1) // 2
    margin = (reach + ROUND - 1) // ROUND * ROUND
    edge = margin * layers
    pieces = 3 * layers
    cores = half // LANES

    me = lax.axis_index("sp")
    core = lax.axis_index("tp")
    z = me // plane
    cell = lax.rem(me, plane)
    side_y = cell // width_x
    side_x = lax.rem(cell, width_x)
    parity = lax.rem(z, 2)
    pair = me + (1 - 2 * parity) * plane
    x_mate = me + 1 - 2 * side_x
    y_mate = me + (1 - 2 * side_y) * width_x
    x_cell = cell + 1 - 2 * side_x
    y_cell = cell + (1 - 2 * side_y) * width_x
    has_low = me > 0
    has_high = me < count - 1
    own_cols = pl.ds(pl.multiple_of(core * wide + parity * half, LANES), half)
    pair_cols = pl.ds(pl.multiple_of(core * wide + (1 - parity) * half, LANES), half)
    mate_cols = pl.ds(pl.multiple_of((1 - core) * wide + parity * half, LANES), half)
    far_cols = pl.ds(pl.multiple_of((1 - core) * wide + (1 - parity) * half, LANES), half)
    core_cols = pl.ds(pl.multiple_of(core * wide, LANES), wide)
    across_cols = pl.ds(pl.multiple_of((1 - core) * wide, LANES), wide)
    half_cols = pl.ds(pl.multiple_of(parity * half, LANES), half)
    far_half_cols = pl.ds(pl.multiple_of((1 - parity) * half, LANES), half)

    def at(chip):
        return {"sp": chip}

    mate = {"tp": 1 - core}
    group = [mate, at(pair), {"sp": pair, "tp": 1 - core}]

    def remote(src, dst, send, recv, device):
        return pltpu.make_async_remote_copy(
            src_ref=src, dst_ref=dst, send_sem=send, recv_sem=recv, device_id=device, device_id_type=MESH
        )

    barrier = pltpu.get_barrier_semaphore()
    friends = [at(lax.rem(me + step * plane, count)) for step in range(1, depth_z)]
    friends += [at(x_mate), at(y_mate), mate, group[2]]
    friends += [at(lax.rem(me + 1, count)), at(lax.rem(me + count - 1, count))]
    for friend in friends:
        pl.semaphore_signal(barrier, inc=1, device_id=friend, device_id_type=MESH)

    pl.semaphore_wait(barrier, len(friends))

    matrices = (a_weight, gate_weight, out_weight)
    mid = depth // 2

    def own_weight(piece):
        return pltpu.make_async_copy(
            matrices[piece % 3].at[piece // 3, :, half_cols], weights.at[piece, z, cell], w_local.at[piece]
        )

    def along_z(piece, step):
        other = lax.rem(z + step, depth_z)
        cols = pl.ds(pl.multiple_of(lax.rem(other, 2) * half, LANES), half)
        return remote(
            matrices[piece % 3].at[piece // 3, :, cols],
            weights.at[piece, z, cell],
            w_send.at[piece, step - 1],
            w_recv.at[piece, step - 1],
            at(lax.rem(me + step * plane, count)),
        )

    def part(piece, which, side):
        block = weights.at[piece, :, which, pl.ds(side * mid, mid), :]
        return block

    base = depth_z - 1

    def in_plane(piece, slot):
        device = at(x_mate) if slot in (0, 1, 5) else at(y_mate)
        which = {4: x_cell, 5: y_cell}.get(slot, cell)
        side = {0: 0, 1: 1, 2: 1, 3: 0, 4: 0, 5: 1}[slot]
        block = part(piece, which, side)
        return remote(block, block, w_send.at[piece, base + slot], w_recv.at[piece, base + slot], device)

    def send_z(piece):
        own_weight(piece).start()
        for step in range(1, depth_z):
            along_z(piece, step).start()

    def spread_plane(piece):
        own_weight(piece).wait()
        for step in range(1, depth_z):
            along_z(piece, step).wait_recv()
        for slot in (0, 2, 1, 3):
            in_plane(piece, slot).start()

    def relay(piece):
        in_plane(piece, 0).wait_recv()
        in_plane(piece, 4).start()
        in_plane(piece, 2).wait_recv()
        in_plane(piece, 5).start()

    def have(piece):
        for slot in (1, 3, 4, 5):
            in_plane(piece, slot).wait_recv()

    lows, mains, highs = pl.ds(0, edge), pl.ds(edge, rows), pl.ds(edge + rows, edge)
    local_stream = pltpu.make_async_copy(stream, spread.at[parity, mains, core_cols], x_local)
    main_pair = remote(stream, spread.at[parity, mains, core_cols], x_send.at[0], x_recv.at[0], at(pair))
    low_pair = remote(
        spread.at[parity, lows, core_cols], spread.at[parity, lows, core_cols], x_send.at[1], x_recv.at[1], at(pair)
    )
    high_pair = remote(
        spread.at[parity, highs, core_cols], spread.at[parity, highs, core_cols], x_send.at[2], x_recv.at[2], at(pair)
    )
    down_parity = lax.rem(lax.max(me - 1, 0) // plane, 2)
    up_parity = lax.rem(lax.min(me + 1, count - 1) // plane, 2)
    to_low = remote(
        stream.at[pl.ds(0, edge)], spread.at[down_parity, highs, core_cols], x_send.at[3], x_recv.at[3], at(me - 1)
    )
    to_high = remote(
        stream.at[pl.ds(rows - edge, edge)], spread.at[up_parity, lows, core_cols], x_send.at[4], x_recv.at[4], at(me + 1)
    )

    def to_mate(which, slot):
        block = spread.at[which, :, core_cols]
        return remote(block, block, x_send.at[slot], x_recv.at[slot], mate)

    local_stream.start()

    @pl.when(has_low)
    def _():
        to_low.start()

    @pl.when(has_high)
    def _():
        to_high.start()

    send_z(0)
    send_z(1)
    main_pair.start()
    send_z(2)
    send_z(3)

    @pl.when(jnp.logical_not(has_low))
    def _():
        spread[parity, lows, core_cols] = jnp.zeros((edge, wide), jnp.bfloat16)

    @pl.when(jnp.logical_not(has_high))
    def _():
        spread[parity, highs, core_cols] = jnp.zeros((edge, wide), jnp.bfloat16)

    for layer in range(layers):
        for c in range(cores):
            cols = pl.ds(pl.multiple_of(parity * half + c * LANES, LANES), LANES)
            taps_own[layer, c, pl.ds(0, taps), :] = conv_weight[layer, :, cols]
            cols_own[layer, 0:1, pl.ds(c * LANES, LANES)] = conv_bias[layer : layer + 1, cols]
            cols_own[layer, 1:2, pl.ds(c * LANES, LANES)] = ln_gain[layer : layer + 1, cols]
            cols_own[layer, 2:3, pl.ds(c * LANES, LANES)] = ln_shift[layer : layer + 1, cols]

    local_stream.wait()

    @pl.when(has_low)
    def _():
        to_high.wait_recv()

    @pl.when(has_high)
    def _():
        to_low.wait_recv()

    low_pair.start()
    high_pair.start()
    to_mate(parity, 5).start()

    def normalize(source, layer, which, start, size):
        gain = norm_gain[layer : layer + 1, :]

        def step(i, carry):
            at_row = pl.multiple_of(start + i * ROUND, ROUND)
            block = source[which, pl.ds(at_row, ROUND), :].astype(jnp.float32)
            factor = lax.rsqrt(jnp.mean(block * block, axis=1, keepdims=True) + EPSILON)
            normed[which, pl.ds(at_row, ROUND), :] = (block * factor * gain).astype(jnp.bfloat16)
            return carry

        lax.fori_loop(0, size // ROUND, step, 0)

    def matrix(piece, col, size):
        return weights[piece, :, :, :, pl.ds(col, size)].reshape(total, size)

    def gate(layer, which, start, size):
        block = normed[which, pl.ds(start, size), :]
        step = 2 * LANES
        for col in range(0, half, step):
            linear = jnp.dot(block, matrix(3 * layer, col, step), preferred_element_type=jnp.float32)
            gating = jnp.dot(block, matrix(3 * layer + 1, col, step), preferred_element_type=jnp.float32)
            value = (linear * jax.nn.sigmoid(gating)).astype(jnp.bfloat16).astype(jnp.float32)
            for c in range(step // LANES):
                gated[which, col // LANES + c, pl.ds(start, size), :] = value[:, c * LANES : (c + 1) * LANES]

    lane = lax.broadcasted_iota(jnp.int32, (8, LANES), 1)

    def convolve_chunk(layer, chunk, which, start, size):
        steps = 2 if size % 16 == 0 else 1
        block_rows = size // steps
        zero = jnp.zeros((8, LANES), jnp.float32)

        def step(i, carry):
            packed, packed_squares = carry
            at_row = pl.multiple_of(start + i * block_rows, 8)
            summed = squares = None
            for c in range(cores):
                acc = jnp.broadcast_to(cols_own[layer, 0:1, c * LANES : (c + 1) * LANES], (block_rows, LANES))
                for k in range(taps):
                    window = gated[which, c, pl.ds(at_row + (margin - reach + k), block_rows), :]
                    acc = acc + window * taps_own[layer, c, k : k + 1, :]
                conv_out[which, c, pl.ds(at_row, block_rows), :] = acc
                summed = acc if summed is None else summed + acc
                squares = acc * acc if squares is None else squares + acc * acc
            summed = jnp.sum(summed, axis=1, keepdims=True)
            squares = jnp.sum(squares, axis=1, keepdims=True)
            for tile in range(block_rows // 8):
                here = lane == i * (block_rows // 8) + tile
                packed = jnp.where(here, summed[8 * tile : 8 * tile + 8], packed)
                packed_squares = jnp.where(here, squares[8 * tile : 8 * tile + 8], packed_squares)
            return packed, packed_squares

        packed, packed_squares = lax.fori_loop(0, steps, step, (zero, zero))
        sums_own[layer, chunk, 0] = packed
        sums_own[layer, chunk, 1] = packed_squares
        for slot in range(RELATIONS):
            send_sums(layer, chunk, slot).start()

    def send_sums(layer, chunk, slot):
        return remote(
            sums_own.at[layer, chunk],
            sums_in.at[layer, chunk, slot],
            s_send.at[layer, chunk, slot],
            s_recv.at[layer, chunk, slot],
            group[slot],
        )

    def block_to(buffer, which, start, size, cols, send, recv, layer, chunk, slot):
        block = buffer.at[which, pl.ds(start, size), cols]
        device = at(pair) if slot == 0 else mate
        return remote(block, block, send.at[layer, chunk, slot], recv.at[layer, chunk, slot], device)

    def mix_chunk(layer, chunk, which, start, size):
        sums = sums_own[layer, chunk]
        for slot in range(RELATIONS):
            send_sums(layer, chunk, slot).wait_recv()
            sums = sums + sums_in[layer, chunk, slot]
        average = sums[0] / total
        scale = lax.rsqrt(sums[1] / total - average * average + EPSILON)
        gain = cols_own[layer, 1:2, :]
        shift = cols_own[layer, 2:3, :]
        for i in range(size // ROUND):
            tiles = [2 * i, 2 * i + 1]
            middle = jnp.concatenate([average[:, t : t + 1] for t in tiles], axis=0)
            factor = jnp.concatenate([scale[:, t : t + 1] for t in tiles], axis=0)
            values = []
            for c in range(cores):
                cols = slice(c * LANES, (c + 1) * LANES)
                value = conv_out[which, c, pl.ds(start + i * ROUND, ROUND), :]
                value = (value - middle) * factor * gain[:, cols] + shift[:, cols]
                values.append((value * jax.nn.sigmoid(value)).astype(jnp.bfloat16))
            mixed[layer][which, pl.ds(start + i * ROUND, ROUND), own_cols] = jnp.concatenate(values, axis=1)
        for slot in (0, 1):
            mixed_copy(layer, chunk, which, start, size, slot).start()

    def mixed_copy(layer, chunk, which, start, size, slot):
        cols = pair_cols if slot == 2 else own_cols
        return block_to(mixed[layer], which, start, size, cols, m_send, m_recv, layer, chunk, slot)

    def inner_copy(layer, chunk, which, start, size, slot):
        cols = pair_cols if slot == 2 else own_cols
        return block_to(inner[layer], which, start, size, cols, c_send, c_recv, layer, chunk, slot)

    def pass_on(copy, *args):
        copy(*args, 0).wait_recv()
        copy(*args, 2).start()

    def arrived(copy, *args):
        copy(*args, 1).wait_recv()
        copy(*args, 2).wait_recv()

    def project(layer, which, start, size):
        block = mixed[layer][which, pl.ds(start, size), :]
        return jnp.dot(block, matrix(3 * layer + 2, 0, half), preferred_element_type=jnp.float32)

    def residual(source, which, start, size):
        return source[which, pl.ds(start + margin, size), own_cols].astype(jnp.float32)

    def send_final(chunk, start, size):
        return remote(
            final.at[pl.ds(start, size), :],
            out.at[pl.ds(start, size), half_cols],
            f_send.at[chunk],
            f_recv.at[chunk],
            at(pair),
        )

    chips = [(z - parity + which) * plane + cell for which in range(2)]

    def finish_chunk(layer, chunk, which, start, size):
        source = spread if layer == 0 else inner[layer - 1]
        value = residual(source, which, start, size) + project(layer, which, start, size)
        if layer == layers - 1:
            value = value.astype(jnp.bfloat16)

            @pl.when(parity == which)
            def _():
                out[pl.ds(start, size), half_cols] = value

            @pl.when(parity != which)
            def _():
                final[pl.ds(start, size), :] = value
                send_final(chunk % CUTS, start, size).start()

            return
        beyond = margin * (layers - 1 - layer)
        index = chips[which] * rows - beyond + start + lax.broadcasted_iota(jnp.int32, (size, 1), 0)
        inside = (index >= 0) & (index < rows * count)
        inner[layer][which, pl.ds(start, size), own_cols] = jnp.where(inside, value, 0.0).astype(jnp.bfloat16)
        for slot in (0, 1):
            inner_copy(layer, chunk, which, start, size, slot).start()

    def chunks_of(layer):
        size = (rows + 2 * margin * (layers - 1 - layer)) // CUTS
        return [(which * CUTS + cut, which, cut * size, size) for which in range(2) for cut in range(CUTS)]

    first_rows = rows + 2 * edge

    spread_plane(0)
    relay(0)
    spread_plane(1)
    relay(1)
    spread_plane(2)

    main_pair.wait_recv()
    low_pair.wait_recv()
    high_pair.wait_recv()
    to_mate(1 - parity, 6).start()
    to_mate(parity, 5).wait_recv()
    to_mate(1 - parity, 6).wait_recv()
    for which in range(2):
        normalize(spread, 0, which, 0, first_rows)
    for layer in range(layers):
        first = 3 * layer
        have(first)
        have(first + 1)
        if layer == 0:
            for which in range(2):
                gate(0, which, 0, first_rows)
        else:
            previous = chunks_of(layer - 1)
            for args in previous:
                pass_on(inner_copy, layer - 1, *args)
                arrived(inner_copy, layer - 1, *args)
                _, which, start, size = args
                normalize(inner[layer - 1], layer, which, start, size)
                gate(layer, which, start, size)
        if layer == 0:
            relay(2)
        current = chunks_of(layer)
        for args in current:
            convolve_chunk(layer, *args)
        if layer == 0:
            spread_plane(3)
        for args in current:
            mix_chunk(layer, *args)
        if layer == 0:
            send_z(4)
            send_z(5)
        have(first + 2)
        for args in current:
            pass_on(mixed_copy, layer, *args)
            arrived(mixed_copy, layer, *args)
            finish_chunk(layer, *args)
            if layer == 0:
                if args[0] == 0:
                    relay(3)
                if args[0] == 1:
                    spread_plane(4)
                if args[0] == 3:
                    relay(4)
                    spread_plane(5)
                    relay(5)

    sends = CUTS
    for cut in range(sends):
        size = rows // CUTS
        send_final(cut, cut * size, size).wait()
    for piece in range(pieces):
        for step in range(1, depth_z):
            along_z(piece, step).wait_send()
        for slot in range(6):
            in_plane(piece, slot).wait_send()
    main_pair.wait_send()
    low_pair.wait_send()
    high_pair.wait_send()
    to_mate(parity, 5).wait_send()
    to_mate(1 - parity, 6).wait_send()

    @pl.when(has_low)
    def _():
        to_low.wait_send()

    @pl.when(has_high)
    def _():
        to_high.wait_send()

    for layer in range(layers):
        for args in chunks_of(layer):
            for slot in range(RELATIONS):
                send_sums(layer, args[0], slot).wait_send()
                mixed_copy(layer, *args, slot).wait_send()
                if layer < layers - 1:
                    inner_copy(layer, *args, slot).wait_send()


def fused(sizes, stream, norm_gain, a_weight, gate_weight, conv_weight, conv_bias, ln_gain, ln_shift, out_weight):
    layers, taps = conv_weight.shape[:2]
    rows, wide = stream.shape
    half = wide // 2
    reach = (taps - 1) // 2
    margin = (reach + ROUND - 1) // ROUND * ROUND
    edge = margin * layers
    total = 2 * wide
    depth = a_weight.shape[1]
    plane = sizes[1] * sizes[2]
    first_rows = rows + 2 * edge
    cores = half // LANES
    pieces = 3 * layers
    outs = [rows + 2 * margin * (layers - 1 - layer) for layer in range(layers)]
    bf16, f32 = jnp.bfloat16, jnp.float32
    scratch = [
        pltpu.VMEM((pieces, sizes[0], plane, depth, half), bf16),
        pltpu.VMEM((2, first_rows, total), bf16),
        pltpu.VMEM((2, first_rows, total), bf16),
        pltpu.VMEM((2, cores, first_rows + 8, LANES), f32),
        pltpu.VMEM((2, cores, outs[0], LANES), f32),
        pltpu.VMEM((rows, half), bf16),
        pltpu.VMEM((layers, cores, (taps + 7) // 8 * 8, LANES), f32),
        pltpu.VMEM((layers, 8, half), f32),
        pltpu.VMEM((layers, 2 * CUTS, 2, 8, LANES), f32),
        pltpu.VMEM((layers, 2 * CUTS, RELATIONS, 2, 8, LANES), f32),
    ]
    scratch += [pltpu.VMEM((2, outs[layer], total), bf16) for layer in range(layers - 1)]
    scratch += [pltpu.VMEM((2, outs[layer], total), bf16) for layer in range(layers)]
    dma = pltpu.SemaphoreType.DMA
    stages = sizes[0] - 1 + 6
    scratch += [dma((pieces,)), dma((pieces, stages)), dma((pieces, stages)), dma]
    scratch += [dma((7,)), dma((7,))]
    scratch += [dma((layers, 2 * CUTS, RELATIONS))] * 6
    scratch += [dma((CUTS,))] * 2
    any_space = pl.BlockSpec(memory_space=pl.ANY)
    vmem = pl.BlockSpec(memory_space=pltpu.VMEM)
    return pl.pallas_call(
        functools.partial(fused_kernel, sizes, layers, taps),
        out_shape=jax.ShapeDtypeStruct((rows, wide), bf16),
        in_specs=[any_space, vmem, any_space, any_space, any_space, vmem, vmem, vmem, vmem],
        out_specs=vmem,
        scratch_shapes=scratch,
        compiler_params=pltpu.CompilerParams(
            collective_id=1, has_side_effects=True, vmem_limit_bytes=VMEM_BYTES
        ),
    )(stream, norm_gain, a_weight, gate_weight, out_weight, conv_weight, conv_bias, ln_gain, ln_shift)


def pairs_along_z(sizes, mesh):
    return sizes[0] % 2 == 0 and sizes[1] == 2 and sizes[2] == 2 and mesh.shape["tp"] == 2


def solution(mesh):
    placed = (
        P("sp", "tp"),
        P(),
        P(None, "sp", "tp"),
        P(None, "sp", "tp"),
        P(None, None, "tp"),
        P(None, "tp"),
        P(None, "tp"),
        P(None, "tp"),
        P(None, "sp", "tp"),
    )
    sizes = grid_of(mesh)
    paired = pairs_along_z(sizes, mesh)

    def whole(*args):
        return fused(sizes, *args) if paired else local(sizes, *args)

    return jax.shard_map(
        whole, mesh=mesh, in_specs=placed, out_specs=P("sp", "tp"), check_vma=False
    )
```
